128 devices in a mesh: fs: 16 (over z, x), tp: 8 (over y, core).
Axes of the slice: x: 4, y: 4, z: 4, core: 2. Of those that a mesh axis runs over, the one named last changes fastest.
Arguments:
- resid: bfloat16 [16384, 2048], P(('fs', 'tp')), may hold values from -6 to 6
- mix_gain: float32 [2048], replicated, may hold values from 0.1 to 1.9
- in_weight: bfloat16 [2048, 2048], P('fs', 'tp'), may hold values from -0.125 to 0.125
- conv_taps: float32 [4, 2048], P(None, 'tp'), may hold values from -3 to 3
- recur_gate_w: bfloat16 [32, 64, 64], P('tp'), may hold values from -0.75 to 0.75
- input_gate_w: bfloat16 [32, 64, 64], P('tp'), may hold values from -0.75 to 0.75
- decay_rate: float32 [2048], P('tp'), may hold values from 0.0004 to 0.03
- out_weight: bfloat16 [2048, 2048], P('tp', 'fs'), may hold values from -0.25 to 0.25
- mlp_gain: float32 [2048], replicated, may hold values from 0.1 to 1.9
- up_gate_w: bfloat16 [2048, 5632], P('fs', 'tp'), may hold values from -0.125 to 0.125
- up_val_w: bfloat16 [2048, 5632], P('fs', 'tp'), may hold values from -0.125 to 0.125
- ffn_taps: float32 [3, 5632], P(None, 'tp'), may hold values from -3 to 3
- down_weight: bfloat16 [5632, 2048], P('tp', 'fs'), may hold values from -0.15625 to 0.15625
Outputs:
- result: bfloat16 [16384, 2048], P(('fs', 'tp'))
The draws below stay inside these ranges and needn't reach their ends.
All inputs are finite; a program needn't handle non-finite values.
Results may differ from the reference program's by a relative error of at most 0.028.
Values may be sent and summed in bfloat16 or wider, within the bound.
No kernel may reach another device: no remote copies, remote signals or barrier semaphores. Data moves between devices by JAX's collectives and lax.ppermute only.
A program may use at most 64 MiB of HBM per device.

```python
import math
import jax
import jax.numpy as jnp
from jax import lax

D = 2048
RECUR = 2048
HIDDEN_SIZE = 5632
GATE_BLOCK = 64
SEQ_LEN = 128
NBLOCKS = 32
TOKENS = 16384
N_TP = 8


def block_levels(stream_key, dims, pieces, low, high):
    gain = 1.0
    for position, parts in pieces:
        heights = jax.random.uniform(jax.random.fold_in(jax.random.fold_in(stream_key, 6), position), (parts,), jnp.float32, low / len(pieces), high / len(pieces))
        gain = gain * jnp.repeat(jnp.exp(heights), dims[position] // parts).reshape((-1,) + (1,) * (len(dims) - 1 - position))
    return gain


def noise(rng, dims, spread, reach, shards=(), kind=jnp.bfloat16):
    level = block_levels(rng, dims, shards, -0.22, 0.18) if shards else 1.0
    drawn = jax.random.normal(rng, dims, jnp.float32) * spread * level
    return jnp.minimum(jnp.maximum(drawn, -reach), reach).astype(kind)


def setup_inputs(seed: int = 0) -> dict:
    splits = jax.random.split(jax.random.key(seed), 14)
    return {
        "resid": noise(splits[0], (TOKENS, D), 1.0, 6.0, ((0, 128),)),
        "mix_gain": jnp.clip(1.0 + 0.18 * jax.random.normal(splits[1], (D,), jnp.float32), 0.1, 1.9),
        "in_weight": noise(splits[2], (D, RECUR), D ** -0.5, 0.125, ((0, 16), (1, 8))),
        "conv_taps": noise(splits[3], (4, RECUR), 0.5, 3.0, ((1, 8),), jnp.float32),
        "recur_gate_w": noise(splits[4], (NBLOCKS, GATE_BLOCK, GATE_BLOCK), GATE_BLOCK ** -0.5, 0.75, ((0, 8),)),
        "input_gate_w": noise(splits[5], (NBLOCKS, GATE_BLOCK, GATE_BLOCK), GATE_BLOCK ** -0.5, 0.75, ((0, 8),)),
        "decay_rate": jnp.clip(jnp.exp(math.log(0.03) - 4.317488 * jax.random.uniform(splits[6], (RECUR,), jnp.float32) ** block_levels(splits[6], (RECUR,), ((0, 8),), -0.2, 0.2)), 0.0004, 0.03),
        "out_weight": noise(splits[7], (RECUR, D), (RECUR // 4) ** -0.5, 0.25, ((0, 8), (1, 16))),
        "mlp_gain": jnp.clip(1.0 + 0.18 * jax.random.normal(splits[8], (D,), jnp.float32), 0.1, 1.9),
        "up_gate_w": noise(splits[9], (D, HIDDEN_SIZE), D ** -0.5, 0.125, ((0, 16), (1, 8))),
        "up_val_w": noise(splits[10], (D, HIDDEN_SIZE), D ** -0.5, 0.125, ((0, 16), (1, 8))),
        "ffn_taps": noise(splits[11], (3, HIDDEN_SIZE), 0.6, 3.0, ((1, 8),), jnp.float32),
        "down_weight": noise(splits[12], (HIDDEN_SIZE, D), (HIDDEN_SIZE // 4) ** -0.5, 0.15625, ((0, 8), (1, 16))),
    }


def rms_scale(rows_in, gain_vec):
    wide = rows_in.astype(jnp.float32)
    return wide * lax.rsqrt(lax.optimization_barrier(jnp.mean(wide * wide, axis=-1, keepdims=True)) + 1e-06) * gain_vec

def causal_taps(values, tap_weights):
    width = tap_weights.shape[0]
    length = values.shape[1]
    padded = jnp.pad(values, ((0, 0), (width - 1, 0), (0, 0)))
    summed = jnp.zeros_like(values)
    for tap_index in range(width):
        summed = summed + padded[:, tap_index:tap_index + length] * tap_weights[tap_index]
    return summed

def combine(earlier, later):
    return (earlier[0] * later[0], later[0] * earlier[1] + later[1])

def group_sum(left, right, groups):
    step_size = left.shape[1] // groups
    summed = jnp.zeros((left.shape[0], right.shape[1]), jnp.float32)
    for group in range(groups):
        term = jnp.dot(left[:, group * step_size:(group + 1) * step_size], right[group * step_size:(group + 1) * step_size], preferred_element_type=jnp.float32)
        term = lax.optimization_barrier(term.astype(jnp.bfloat16))
        summed = summed + term.astype(jnp.float32)
    return summed

def reference(resid, mix_gain, in_weight, conv_taps, recur_gate_w, input_gate_w, decay_rate, out_weight, mlp_gain, up_gate_w, up_val_w, ffn_taps, down_weight):
    seqs = TOKENS // SEQ_LEN
    normed = rms_scale(resid, mix_gain).astype(jnp.bfloat16)
    projected = jnp.dot(normed, in_weight, preferred_element_type=jnp.float32).astype(jnp.bfloat16)
    conv = causal_taps(projected.astype(jnp.float32).reshape(seqs, SEQ_LEN, RECUR), conv_taps)
    blocks = conv.astype(jnp.bfloat16).astype(jnp.float32).reshape(seqs, SEQ_LEN, NBLOCKS, GATE_BLOCK)
    rgate = jax.nn.sigmoid(jnp.einsum('slnd,nde->slne', blocks, recur_gate_w.astype(jnp.float32)).reshape(seqs, SEQ_LEN, RECUR))
    igate = jax.nn.sigmoid(jnp.einsum('slnd,nde->slne', blocks, input_gate_w.astype(jnp.float32)).reshape(seqs, SEQ_LEN, RECUR))
    logdecay = -8.0 * rgate * decay_rate
    decay = jnp.exp(logdecay)
    drive = jnp.sqrt(-jnp.expm1(2.0 * logdecay)) * (igate * conv)
    state = lax.associative_scan(combine, (decay, drive), axis=1)[1]
    recurred = state.astype(jnp.bfloat16).reshape(TOKENS, RECUR)
    mixed_sum = group_sum(recurred, out_weight, N_TP)
    middle = (resid.astype(jnp.float32) + mixed_sum).astype(jnp.bfloat16)
    normed_two = rms_scale(middle, mlp_gain).astype(jnp.bfloat16)
    gate_pre = jnp.dot(normed_two, up_gate_w, preferred_element_type=jnp.float32).astype(jnp.bfloat16)
    value_pre = jnp.dot(normed_two, up_val_w, preferred_element_type=jnp.float32).astype(jnp.bfloat16)
    gate_conv = causal_taps(gate_pre.astype(jnp.float32).reshape(seqs, SEQ_LEN, HIDDEN_SIZE), ffn_taps).reshape(TOKENS, HIDDEN_SIZE)
    hidden = (jax.nn.silu(gate_conv) * value_pre.astype(jnp.float32)).astype(jnp.bfloat16)
    ffn_sum = group_sum(hidden, down_weight, N_TP)
    return (middle.astype(jnp.float32) + ffn_sum).astype(jnp.bfloat16)
```

```python
import jax
import jax.numpy as jnp
from jax import lax
from jax.experimental import pallas as pl
from jax.experimental.pallas import tpu as pltpu
from jax.sharding import Mesh
from jax.sharding import PartitionSpec as P

SEQ = 128
D = 2048
BLK = 128
F32 = jnp.float32
BF16 = jnp.bfloat16
MIB = 1024 * 1024
FS = ("z", "x")
TP = ("y", "c")
FS_TP = ("z", "x", "y", "c")


def fetch(a, axis, ahead):
    size = lax.axis_size(axis)
    return lax.ppermute(a, axis, [(i, (i - ahead) % size) for i in range(size)])


def fetch_all(a, axis):
    one, three, two = fetch(a, axis, 1), fetch(a, axis, 3), fetch(a, axis, 2)
    return [a, one, two, three]


def partner(a):
    return fetch(a, "c", 1)


def call(body, out, vmem_mib, *args, flops=0):
    def bytes_of(s):
        return s.size * s.dtype.itemsize

    outs = out if isinstance(out, (list, tuple)) else [out]
    moved = sum(bytes_of(a) for a in args) + sum(bytes_of(o) for o in outs)
    return pl.pallas_call(
        body,
        out_shape=out,
        compiler_params=pltpu.CompilerParams(vmem_limit_bytes=vmem_mib * MIB),
        cost_estimate=pl.CostEstimate(flops=flops, transcendentals=0, bytes_accessed=moved),
    )(*args)


def sds(shape, dtype=BF16):
    return jax.ShapeDtypeStruct(shape, dtype)


def first_norm_body(order, resid, gain, gain2, resid_rel, normed_rel, gain2_rel):
    wide = resid[...].astype(F32)
    scale = lax.rsqrt(jnp.mean(wide * wide, axis=-1, keepdims=True) + 1e-06)
    for j in range(D // BLK):
        at = pl.multiple_of(order[j] * BLK, BLK)
        block = resid[:, pl.ds(at, BLK)]
        put = slice(j * BLK, (j + 1) * BLK)
        resid_rel[:, put] = block
        normed_rel[:, put] = (block.astype(F32) * scale * gain[:, pl.ds(at, BLK)]).astype(BF16)
        gain2_rel[:, put] = gain2[:, pl.ds(at, BLK)]


def first_norm(order, resid, gain, gain2):
    vm = pl.BlockSpec(memory_space=pltpu.VMEM)
    return pl.pallas_call(
        first_norm_body,
        in_specs=[pl.BlockSpec(memory_space=pltpu.SMEM), vm, vm, vm],
        out_shape=[sds((SEQ, D)), sds((SEQ, D)), sds((1, D), F32)],
        compiler_params=pltpu.CompilerParams(vmem_limit_bytes=8 * MIB),
    )(order, resid, gain.reshape(1, D), gain2.reshape(1, D))


def second_norm_body(resid, p0, p1, p2, p3, gain, middle, normed):
    total = (p0[...].astype(F32) + p1[...].astype(F32)) + (p2[...].astype(F32) + p3[...].astype(F32))
    mid = (resid[...].astype(F32) + total).astype(BF16)
    middle[...] = mid
    wide = mid.astype(F32)
    scale = lax.rsqrt(jnp.mean(wide * wide, axis=-1, keepdims=True) + 1e-06)
    normed[...] = (wide * scale * gain[...]).astype(BF16)


def last_sum_body(order, middle, p0, p1, p2, p3, out):
    for j in range(D // BLK):
        at = pl.multiple_of(order[j] * BLK, BLK)
        put = slice(j * BLK, (j + 1) * BLK)
        total = (p0[:, put].astype(F32) + p1[:, put].astype(F32)) + (
            p2[:, put].astype(F32) + p3[:, put].astype(F32)
        )
        out[:, pl.ds(at, BLK)] = (middle[:, put].astype(F32) + total).astype(BF16)


def last_sum(order, middle, parts):
    vm = pl.BlockSpec(memory_space=pltpu.VMEM)
    return pl.pallas_call(
        last_sum_body,
        in_specs=[pl.BlockSpec(memory_space=pltpu.SMEM)] + [vm] * 5,
        out_shape=sds((SEQ, D)),
        compiler_params=pltpu.CompilerParams(vmem_limit_bytes=8 * MIB),
    )(order, middle, *parts)


def delayed(v, steps, rows, fill):
    return jnp.where(rows >= steps, pltpu.roll(v, steps, 0), fill)


def sigmoid(v):
    return 1.0 / (1.0 + jnp.exp(-v))


def minus_expm1(v, exp_v):
    series = jnp.full_like(v, 1.0 / 9.0)
    series = 1.0 + v * series
    for k in (8.0, 7.0, 6.0, 5.0, 4.0, 3.0, 2.0):
        series = 1.0 + v * series * (1.0 / k)
    return jnp.where(v > -0.5, -v * series, 1.0 - exp_v)


def mix_body(x, in_own, in_par, taps, gates, rate, out_own, out_par, out):
    xs = x[...]
    rows = lax.broadcasted_iota(jnp.int32, (SEQ, BLK), 0)
    states = []
    for half, w in enumerate((in_own, in_par)):
        wide = jnp.dot(xs, w[...], preferred_element_type=F32).astype(BF16).astype(F32)
        for t in range(2):
            tile = half * 2 + t
            cols = slice(tile * BLK, (tile + 1) * BLK)
            p = wide[:, t * BLK : (t + 1) * BLK]
            conv = p * taps[3:4, cols]
            for k in range(3):
                conv = conv + delayed(p, 3 - k, rows, 0.0) * taps[k : k + 1, cols]
            g = jnp.dot(conv.astype(BF16), gates[tile], preferred_element_type=F32)
            rgate = sigmoid(g[:, :BLK])
            igate = sigmoid(g[:, BLK:])
            logdecay = -8.0 * rgate * rate[:, cols]
            a = jnp.exp(logdecay)
            b = jnp.sqrt(minus_expm1(2.0 * logdecay, a * a)) * (igate * conv)
            step = 1
            while step < SEQ:
                b = a * delayed(b, step, rows, 0.0) + b
                if step * 2 < SEQ:
                    a = a * delayed(a, step, rows, 1.0)
                step *= 2
            states.append(b.astype(BF16))
    left = jnp.concatenate(states[:2], axis=1)
    right = jnp.concatenate(states[2:], axis=1)
    for n in range(4):
        cols = slice(n * 512, (n + 1) * 512)
        part = jnp.dot(left, out_own[:, cols], preferred_element_type=F32)
        part = part + jnp.dot(right, out_par[:, cols], preferred_element_type=F32)
        out[:, cols] = part.astype(BF16)


def ffn_body(x, ua_own, ub_own, ua_par, ub_par, taps, down, out):
    xs = x[...]
    rows = lax.broadcasted_iota(jnp.int32, (SEQ, BLK), 0)
    lanes = lax.broadcasted_iota(jnp.int32, (SEQ, BLK), 1)

    def tap3(g, tile):
        cols = slice(tile * BLK, (tile + 1) * BLK)
        conv = g * taps[2:3, cols]
        for k in range(2):
            conv = conv + delayed(g, 2 - k, rows, 0.0) * taps[k : k + 1, cols]
        return conv

    def gated(g, v, tile):
        g = g.astype(BF16).astype(F32)
        v = v.astype(BF16).astype(F32)
        c = tap3(g, tile)
        return (c * sigmoid(c) * v).astype(BF16)

    hidden = []
    ends = []
    for half, (ua, ub) in enumerate(((ua_own, ub_own), (ua_par, ub_par))):
        ya = jnp.dot(xs, ua[...], preferred_element_type=F32)
        yb = jnp.dot(xs, ub[...], preferred_element_type=F32)
        y = [ya[:, t * BLK : (t + 1) * BLK] for t in range(6)]
        y += [yb[:, t * BLK : (t + 1) * BLK] for t in range(5)]
        for t in range(5):
            hidden.append(gated(y[t], y[5 + t], half * 5 + t))
        ends.append(y[10])
    low = lanes < 64
    g_end = jnp.where(low, ends[0], pltpu.roll(ends[1], 64, 1))
    v_end = jnp.where(low, pltpu.roll(ends[0], 64, 1), ends[1])
    hidden.append(gated(g_end, v_end, 10))
    h = jnp.concatenate(hidden, axis=1)
    for n in range(4):
        cols = slice(n * 512, (n + 1) * 512)
        out[:, cols] = jnp.dot(h, down[:, cols], preferred_element_type=F32).astype(BF16)


def exchanged_sums(parts):
    return [parts[0], fetch(parts[3], "y", 1), fetch(parts[2], "y", 2), fetch(parts[1], "y", 3)]


def shards(
    resid,
    mix_gain,
    in_weight,
    conv_taps,
    recur_gate_w,
    input_gate_w,
    decay_rate,
    out_weight,
    mlp_gain,
    up_gate_w,
    up_val_w,
    ffn_taps,
    down_weight,
):
    z, x = lax.axis_index("z"), lax.axis_index("x")
    steps = jnp.arange(16, dtype=jnp.int32)
    order = ((steps // 4 + z) % 4) * 4 + (steps % 4 + x) % 4

    resid_rel, normed, gain2 = first_norm(order, resid, mix_gain, mlp_gain)
    rows1 = fetch_all(normed, "y")

    a = jnp.concatenate([in_weight[:, :BLK], out_weight[:BLK]], axis=0)
    b = jnp.concatenate([in_weight[:, BLK:], out_weight[BLK:]], axis=0)
    a = jnp.stack(fetch_all(a, "x"))
    b = jnp.stack(fetch_all(b, "z"))
    a = jnp.stack(fetch_all(a, "z"))
    b = jnp.stack(fetch_all(b, "x"), axis=1)
    a = a.reshape(16, 256, BLK)
    b = b.reshape(16, 256, BLK)
    in_own = jnp.concatenate([a[:, :BLK].reshape(D, BLK), b[:, :BLK].reshape(D, BLK)], axis=1)
    out_own = jnp.concatenate(
        [
            jnp.concatenate([v[i, BLK:] for i in range(16)], axis=1)
            for v in (a, b)
        ],
        axis=0,
    )
    in_par, out_par = partner(in_own), partner(out_own)

    gates = jnp.stack([recur_gate_w, input_gate_w])
    gates = jnp.concatenate([gates, partner(gates)], axis=1).reshape(2, 4, 2, 64, 64)
    zero = jnp.zeros_like(gates[:, :, 0])
    gates = jnp.concatenate(
        [
            jnp.concatenate([gates[:, :, 0], zero], axis=3),
            jnp.concatenate([zero, gates[:, :, 1]], axis=3),
        ],
        axis=2,
    )
    gates = jnp.concatenate([gates[0], gates[1]], axis=2)
    small = jnp.concatenate([conv_taps, decay_rate[None]], axis=0)
    small = jnp.concatenate([small, partner(small)], axis=1)
    taps, rate = small[:4], small[4:]
    ftaps_par = partner(ffn_taps)
    ftaps = jnp.concatenate(
        [ffn_taps[:, :640], ftaps_par[:, :640], ffn_taps[:, 640:], ftaps_par[:, 640:]], axis=1
    )

    down_blocks = [down_weight[k * BLK : (k + 1) * BLK] for k in range(5)]
    down_end = jnp.concatenate([down_weight[640:], jnp.zeros((64, BLK), BF16)], axis=0)
    a = jnp.concatenate([up_gate_w[:, :640], up_val_w[:, :BLK], *down_blocks[:2]], axis=1)
    b = jnp.concatenate(
        [up_val_w[:, BLK:640], up_gate_w[:, 640:], up_val_w[:, 640:], *down_blocks[2:], down_end],
        axis=1,
    )
    a = fetch_all(a, "x")
    b = fetch_all(b, "z")
    ua = jnp.concatenate([v[:, :768] for v in a], axis=0)
    ub = jnp.stack([v[:, :640] for v in b])
    ua = jnp.concatenate(fetch_all(ua, "z"), axis=0)
    ub = jnp.stack(fetch_all(ub, "x"), axis=1).reshape(D, 640)
    ua_par, ub_par = partner(ua), partner(ub)
    da = jnp.concatenate(
        [jnp.concatenate([v[:, 768:896], v[:, 896:]], axis=0) for v in a], axis=1
    )
    db = jnp.stack(
        [
            jnp.concatenate(
                [v[:, 640:768], v[:, 768:896], v[:, 896:1024], v[:64, 1024:]], axis=0
            )
            for v in b
        ]
    )
    da = jnp.concatenate(fetch_all(da, "z"), axis=1)
    db = fetch_all(db, "x")
    db = jnp.concatenate([db[j][i] for i in range(4) for j in range(4)], axis=1)
    da_par, db_par = partner(da), partner(db)
    down = jnp.concatenate([da, db[:384], da_par, db_par[:384], db[384:], db_par[384:]], axis=0)

    mixed = [
        call(
            mix_body,
            sds((SEQ, D)),
            24,
            rows,
            in_own,
            in_par,
            taps,
            gates,
            rate,
            out_own,
            out_par,
            flops=2 * SEQ * D * 512 * 2,
        )
        for rows in rows1
    ]
    middle, normed_two = call(
        second_norm_body,
        [sds((SEQ, D)), sds((SEQ, D))],
        8,
        resid_rel,
        *exchanged_sums(mixed),
        gain2,
    )
    rows2 = fetch_all(normed_two, "y")
    fed = [
        call(
            ffn_body,
            sds((SEQ, D)),
            40,
            rows,
            ua,
            ub,
            ua_par,
            ub_par,
            ftaps,
            down,
            flops=2 * SEQ * D * 1408 * 3,
        )
        for rows in rows2
    ]
    return last_sum(order, middle, exchanged_sums(fed))


def solution(mesh):
    split = Mesh(mesh.devices.reshape(4, 4, 4, 2), FS_TP)
    return jax.shard_map(
        shards,
        mesh=split,
        in_specs=(
            P(FS_TP, None),
            P(),
            P(FS, TP),
            P(None, TP),
            P(TP, None, None),
            P(TP, None, None),
            P(TP),
            P(TP, FS),
            P(),
            P(FS, TP),
            P(FS, TP),
            P(None, TP),
            P(TP, FS),
        ),
        out_specs=P(FS_TP, None),
        check_vma=False,
    )
```

```python
import jax
import jax.numpy as jnp
from jax import lax
from jax.experimental import pallas as pl
from jax.experimental.pallas import tpu as pltpu
from jax.sharding import Mesh
from jax.sharding import PartitionSpec as P


SEQ = 128
D = 2048
BLK = 128
HID = 704
F32 = jnp.float32
BF16 = jnp.bfloat16
MIB = 1024 * 1024
FS = ("z", "x")
TP = ("y", "c")
FS_TP = ("z", "x", "y", "c")


def fetch(a, axis, ahead):
    size = lax.axis_size(axis)
    return lax.ppermute(a, axis, [(i, (i - ahead) % size) for i in range(size)])


def fetch_all(a, axis):
    return [a] + [fetch(a, axis, k) for k in (1, 2, 3)]


def partner(a):
    return fetch(a, "c", 1)


VM = pl.BlockSpec(memory_space=pltpu.VMEM)
SM = pl.BlockSpec(memory_space=pltpu.SMEM)


def call(body, out, *args, vmem=4, scalars=0, flops=0, scratch=()):
    return pl.pallas_call(
        body,
        in_specs=[SM] * scalars + [VM] * (len(args) - scalars),
        out_shape=out,
        scratch_shapes=[pltpu.VMEM(*v) for v in scratch],
        compiler_params=pltpu.CompilerParams(vmem_limit_bytes=vmem * MIB),
        cost_estimate=pl.CostEstimate(
            flops=flops, transcendentals=0, bytes_accessed=0
        ),
    )(*args)


def sds(shape, dtype=BF16):
    return jax.ShapeDtypeStruct(shape, dtype)


def first_body(order, resid, gain, gain2, in_w, out_w, resid_rel, normed_rel, gain2_rel, a, b):
    wide = resid[...].astype(F32)
    scale = lax.rsqrt(jnp.mean(wide * wide, axis=-1, keepdims=True) + 1e-06)
    for j in range(D // BLK):
        at = pl.multiple_of(order[j] * BLK, BLK)
        block = resid[:, pl.ds(at, BLK)]
        put = slice(j * BLK, (j + 1) * BLK)
        resid_rel[:, put] = block
        normed_rel[:, put] = (block.astype(F32) * scale * gain[:, pl.ds(at, BLK)]).astype(BF16)
        gain2_rel[:, put] = gain2[:, pl.ds(at, BLK)]
    for half, dst in enumerate((a, b)):
        dst[:BLK] = in_w[:, half * BLK : (half + 1) * BLK]
        dst[BLK:] = out_w[half * BLK : (half + 1) * BLK]


def halves_body(gate, val, down, a, b):
    a[:HID] = gate[...]
    a[HID:] = down[: HID // 2]
    b[:HID] = val[...]
    b[HID:] = down[HID // 2 :]


def second_norm_body(resid, p0, p1, p2, p3, gain, middle, normed):
    total = (p0[...].astype(F32) + p1[...].astype(F32)) + (p2[...].astype(F32) + p3[...].astype(F32))
    mid = (resid[...].astype(F32) + total).astype(BF16)
    middle[...] = mid
    wide = mid.astype(F32)
    scale = lax.rsqrt(jnp.mean(wide * wide, axis=-1, keepdims=True) + 1e-06)
    normed[...] = (wide * scale * gain[...]).astype(BF16)


def last_sum_body(order, middle, p0, p1, p2, p3, out):
    for j in range(D // BLK):
        at = pl.multiple_of(order[j] * BLK, BLK)
        put = slice(j * BLK, (j + 1) * BLK)
        total = (p0[:, put].astype(F32) + p1[:, put].astype(F32)) + (
            p2[:, put].astype(F32) + p3[:, put].astype(F32)
        )
        out[:, pl.ds(at, BLK)] = (middle[:, put].astype(F32) + total).astype(BF16)


def delayed(v, steps, rows, fill):
    return jnp.where(rows >= steps, pltpu.roll(v, steps, 0), fill)


def sigmoid(v):
    return 1.0 / (1.0 + jnp.exp(-v))


def minus_expm1(v, exp_v):
    series = jnp.full_like(v, 1.0 / 9.0)
    series = 1.0 + v * series
    for k in (8.0, 7.0, 6.0, 5.0, 4.0, 3.0, 2.0):
        series = 1.0 + v * series * (1.0 / k)
    return jnp.where(v > -0.5, -v * series, 1.0 - exp_v)


def mix_body(x, in_own, in_par, taps, gates, rate, out_own, out_par, out, proj, states):
    rows = lax.broadcasted_iota(jnp.int32, (SEQ, BLK), 0)
    for half, w in enumerate((in_own, in_par)):
        proj[:, half * 256 : (half + 1) * 256] = jnp.dot(
            x[...], w[...], preferred_element_type=F32
        ).astype(BF16)

    def tile(t, carry):
        cols = pl.ds(pl.multiple_of(t * BLK, BLK), BLK)
        p = proj[:, cols].astype(F32)
        conv = p * taps[3:4, cols]
        for k in range(3):
            conv = conv + delayed(p, 3 - k, rows, 0.0) * taps[k : k + 1, cols]
        g = jnp.dot(conv.astype(BF16), gates[t], preferred_element_type=F32)
        rgate = sigmoid(g[:, :BLK])
        igate = sigmoid(g[:, BLK:])
        logdecay = -8.0 * rgate * rate[:, cols]
        a = jnp.exp(logdecay)
        b = jnp.sqrt(minus_expm1(2.0 * logdecay, a * a)) * (igate * conv)
        step = 1
        while step < SEQ:
            b = a * delayed(b, step, rows, 0.0) + b
            if step * 2 < SEQ:
                a = a * delayed(a, step, rows, 1.0)
            step *= 2
        states[:, cols] = b.astype(BF16)
        return carry

    lax.fori_loop(0, 4, tile, 0)

    def column(n, carry):
        cols = pl.ds(pl.multiple_of(n * 512, 512), 512)
        part = jnp.dot(states[:, :256], out_own[:, cols], preferred_element_type=F32)
        part = part + jnp.dot(states[:, 256:], out_par[:, cols], preferred_element_type=F32)
        out[:, cols] = part.astype(BF16)
        return carry

    lax.fori_loop(0, 4, column, 0)


def nt_dot(a, b):
    return lax.dot_general(a, b, (((1,), (1,)), ((), ())), preferred_element_type=F32)


def up_body(x, gate, val, taps, out):
    rows = lax.broadcasted_iota(jnp.int32, (SEQ, BLK), 0)

    def tile(t, carry):
        cols = pl.ds(pl.multiple_of(t * BLK, BLK), BLK)
        both = nt_dot(x[...], jnp.concatenate([gate[cols], val[cols]], axis=0))
        both = both.astype(BF16).astype(F32)
        g, v = both[:, :BLK], both[:, BLK:]
        conv = g * taps[2:3, cols]
        for k in range(2):
            conv = conv + delayed(g, 2 - k, rows, 0.0) * taps[k : k + 1, cols]
        out[:, cols] = (conv * sigmoid(conv) * v).astype(BF16)
        return carry

    lax.fori_loop(0, 2 * HID // BLK, tile, 0)


def down_body(h, down, out):
    def tile(n, carry):
        cols = pl.ds(pl.multiple_of(n * 512, 512), 512)
        out[:, cols] = jnp.dot(h[...], down[:, cols], preferred_element_type=F32).astype(BF16)
        return carry

    lax.fori_loop(0, 4, tile, 0)


def sums_sent(part, ahead):
    return fetch(part, "y", (-ahead) % 4)


def in_lanes(pieces):
    return jnp.concatenate(pieces, axis=1)


def layer(
    resid,
    mix_gain,
    in_weight,
    conv_taps,
    recur_gate_w,
    input_gate_w,
    decay_rate,
    out_weight,
    mlp_gain,
    up_gate_w,
    up_val_w,
    ffn_taps,
    down_weight,
):
    z, x = lax.axis_index("z"), lax.axis_index("x")
    steps = jnp.arange(16, dtype=jnp.int32)
    order = ((steps // 4 + z) % 4) * 4 + (steps % 4 + x) % 4

    resid_rel, normed, gain2, a, b = call(
        first_body,
        [sds((SEQ, D)), sds((SEQ, D)), sds((1, D), F32), sds((256, BLK)), sds((256, BLK))],
        order,
        resid,
        mix_gain.reshape(1, D),
        mlp_gain.reshape(1, D),
        in_weight,
        out_weight,
        scalars=1,
    )
    rows1 = fetch_all(normed, "y")

    a = jnp.stack(fetch_all(a, "x"))
    b = jnp.stack(fetch_all(b, "z"))
    a = fetch_all(a, "z")
    b = fetch_all(b, "x")
    a = [a[i][j] for i in range(4) for j in range(4)]
    b = [b[j][i] for i in range(4) for j in range(4)]
    in_own = jnp.concatenate(
        [jnp.concatenate([v[:BLK] for v in h], axis=0) for h in (a, b)], axis=1
    )
    out_own = jnp.concatenate([in_lanes([v[BLK:] for v in h]) for h in (a, b)], axis=0)
    in_par, out_par = partner(in_own), partner(out_own)

    gates = jnp.stack([recur_gate_w, input_gate_w])
    gates = jnp.concatenate([gates, partner(gates)], axis=1).reshape(2, 4, 2, 64, 64)
    zero = jnp.zeros_like(gates[:, :, 0])
    gates = jnp.concatenate(
        [
            jnp.concatenate([gates[:, :, 0], zero], axis=3),
            jnp.concatenate([zero, gates[:, :, 1]], axis=3),
        ],
        axis=2,
    )
    gates = jnp.concatenate([gates[0], gates[1]], axis=2)
    small = jnp.concatenate([conv_taps, decay_rate[None]], axis=0)
    small = jnp.concatenate([small, partner(small)], axis=1)
    taps, rate = small[:4], small[4:]
    ftaps = jnp.concatenate([ffn_taps, partner(ffn_taps)], axis=1)

    a, b = call(
        halves_body, [sds((1056, BLK)), sds((1056, BLK))], up_gate_w.T, up_val_w.T, down_weight
    )
    a = fetch_all(a, "x")
    b = fetch_all(b, "z")
    gate = in_lanes(fetch_all(in_lanes([v[:HID] for v in a]), "z"))
    val = fetch_all(jnp.stack([v[:HID] for v in b]), "x")
    val = in_lanes([val[j][i] for i in range(4) for j in range(4)])
    down_a = in_lanes(fetch_all(in_lanes([v[HID:] for v in a]), "z"))
    down_b = fetch_all(jnp.stack([v[HID:] for v in b]), "x")
    down_b = in_lanes([down_b[j][i] for i in range(4) for j in range(4)])
    down = jnp.concatenate([down_a, down_b], axis=0)
    gate = jnp.concatenate([gate, partner(gate)], axis=0)
    val = jnp.concatenate([val, partner(val)], axis=0)
    down = jnp.concatenate([down, partner(down)], axis=0)

    parts = [None] * 4
    for j in (1, 3, 2, 0):
        part = call(
            mix_body,
            sds((SEQ, D)),
            rows1[j],
            in_own,
            in_par,
            taps,
            gates,
            rate,
            out_own,
            out_par,
            flops=2 * SEQ * D * 512 * 2,
            scratch=[((SEQ, 512), BF16), ((SEQ, 512), BF16)],
        )
        parts[j] = sums_sent(part, j) if j else part
    middle, normed_two = call(
        second_norm_body, [sds((SEQ, D)), sds((SEQ, D))], resid_rel, *parts, gain2
    )
    rows2 = fetch_all(normed_two, "y")
    for j in (0, 1, 3, 2):
        hidden = call(
            up_body, sds((SEQ, 2 * HID)), rows2[j], gate, val, ftaps, flops=2 * SEQ * D * 1408 * 2
        )
        part = call(down_body, sds((SEQ, D)), hidden, down, flops=2 * SEQ * D * 1408)
        parts[j] = sums_sent(part, j) if j else part
    return call(last_sum_body, sds((SEQ, D)), order, middle, *parts, scalars=1)


def solution(mesh):
    split = Mesh(mesh.devices.reshape(4, 4, 4, 2), FS_TP)
    return jax.shard_map(
        layer,
        mesh=split,
        in_specs=(
            P(FS_TP, None),
            P(),
            P(FS, TP),
            P(None, TP),
            P(TP, None, None),
            P(TP, None, None),
            P(TP),
            P(TP, FS),
            P(),
            P(FS, TP),
            P(FS, TP),
            P(None, TP),
            P(TP, FS),
        ),
        out_specs=P(FS_TP, None),
        check_vma=False,
    )
```

```python
import jax
import jax.numpy as jnp
from jax import lax
from jax.experimental import pallas as pl
from jax.experimental.pallas import tpu as pltpu
from jax.sharding import Mesh
from jax.sharding import PartitionSpec as P


SEQ = 128
D = 2048
BLK = 128
HID = 704
F32 = jnp.float32
BF16 = jnp.bfloat16
MIB = 1024 * 1024
FS = ("z", "x")
TP = ("y", "c")
FS_TP = ("z", "x", "y", "c")


def fetch(a, axis, ahead):
    size = lax.axis_size(axis)
    return lax.ppermute(a, axis, [(i, (i - ahead) % size) for i in range(size)])


def fetch_all(a, axis):
    return [a] + [fetch(a, axis, k) for k in (1, 2, 3)]


def partner(a):
    return fetch(a, "c", 1)


VM = pl.BlockSpec(memory_space=pltpu.VMEM)
SM = pl.BlockSpec(memory_space=pltpu.SMEM)
ANY = pl.BlockSpec(memory_space=pl.ANY)


def call(body, out, *args, vmem=4, scalars=0, flops=0, scratch=(), where=VM):
    return pl.pallas_call(
        body,
        in_specs=[SM] * scalars + [where] * (len(args) - scalars),
        out_specs=jax.tree.map(lambda _: VM, out),
        out_shape=out,
        scratch_shapes=scratch,
        compiler_params=pltpu.CompilerParams(vmem_limit_bytes=vmem * MIB),
        cost_estimate=pl.CostEstimate(flops=flops, transcendentals=0, bytes_accessed=0),
    )(*args)


def sds(shape, dtype=BF16):
    return jax.ShapeDtypeStruct(shape, dtype)


def first_body(
    order, resid_h, gain_h, gain2_h, in_h, out_h, gate_h, val_h, down_h,
    resid_rel, normed_rel, gain2_rel, a, b, resid, gain, gain2, sems,
):
    copies = [
        pltpu.make_async_copy(src, dst, sems.at[i])
        for i, (src, dst) in enumerate(
            [
                (resid_h, resid),
                (gain_h, gain),
                (gain2_h, gain2),
                (in_h.at[:, :BLK], a.at[:BLK]),
                (in_h.at[:, BLK:], b.at[:BLK]),
                (out_h.at[:BLK], a.at[BLK : 2 * BLK]),
                (out_h.at[BLK:], b.at[BLK : 2 * BLK]),
                (gate_h, a.at[256 : 256 + HID]),
                (val_h, b.at[256 : 256 + HID]),
                (down_h.at[: HID // 2], a.at[256 + HID :]),
                (down_h.at[HID // 2 :], b.at[256 + HID :]),
            ]
        )
    ]
    for c in copies:
        c.start()
    for c in copies[:3]:
        c.wait()
    wide = resid[...].astype(F32)
    scale = lax.rsqrt(jnp.mean(wide * wide, axis=-1, keepdims=True) + 1e-06)
    for j in range(D // BLK):
        at = pl.multiple_of(order[j] * BLK, BLK)
        block = resid[:, pl.ds(at, BLK)]
        put = slice(j * BLK, (j + 1) * BLK)
        resid_rel[:, put] = block
        normed_rel[:, put] = (block.astype(F32) * scale * gain[:, pl.ds(at, BLK)]).astype(BF16)
        gain2_rel[:, put] = gain2[:, pl.ds(at, BLK)]
    for c in copies[3:]:
        c.wait()


def second_norm_body(resid, p0, p1, p2, p3, gain, middle, normed):
    total = (p0[...].astype(F32) + p1[...].astype(F32)) + (p2[...].astype(F32) + p3[...].astype(F32))
    mid = (resid[...].astype(F32) + total).astype(BF16)
    middle[...] = mid
    wide = mid.astype(F32)
    scale = lax.rsqrt(jnp.mean(wide * wide, axis=-1, keepdims=True) + 1e-06)
    normed[...] = (wide * scale * gain[...]).astype(BF16)


def last_sum_body(order, middle, p0, p1, p2, p3, out):
    for j in range(D // BLK):
        at = pl.multiple_of(order[j] * BLK, BLK)
        put = slice(j * BLK, (j + 1) * BLK)
        total = (p0[:, put].astype(F32) + p1[:, put].astype(F32)) + (
            p2[:, put].astype(F32) + p3[:, put].astype(F32)
        )
        out[:, pl.ds(at, BLK)] = (middle[:, put].astype(F32) + total).astype(BF16)


def delayed(v, steps, rows, fill):
    return jnp.where(rows >= steps, pltpu.roll(v, steps, 0), fill)


def sigmoid(v):
    return 1.0 / (1.0 + jnp.exp(-v))


def minus_expm1(v, exp_v):
    series = jnp.full_like(v, 1.0 / 9.0)
    series = 1.0 + v * series
    for k in (8.0, 7.0, 6.0, 5.0, 4.0, 3.0, 2.0):
        series = 1.0 + v * series * (1.0 / k)
    return jnp.where(v > -0.5, -v * series, 1.0 - exp_v)


def mix_body(x, in_own, in_par, taps, gates, rate, out_own, out_par, out, proj, states):
    rows = lax.broadcasted_iota(jnp.int32, (SEQ, BLK), 0)
    for half, w in enumerate((in_own, in_par)):
        proj[:, half * 256 : (half + 1) * 256] = jnp.dot(
            x[...], w[...], preferred_element_type=F32
        ).astype(BF16)

    def tile(t, carry):
        cols = pl.ds(pl.multiple_of(t * BLK, BLK), BLK)
        p = proj[:, cols].astype(F32)
        conv = p * taps[3:4, cols]
        for k in range(3):
            conv = conv + delayed(p, 3 - k, rows, 0.0) * taps[k : k + 1, cols]
        g = jnp.dot(conv.astype(BF16), gates[t], preferred_element_type=F32)
        rgate = sigmoid(g[:, :BLK])
        igate = sigmoid(g[:, BLK:])
        logdecay = -8.0 * rgate * rate[:, cols]
        a = jnp.exp(logdecay)
        b = jnp.sqrt(minus_expm1(2.0 * logdecay, a * a)) * (igate * conv)
        step = 1
        while step < SEQ:
            b = a * delayed(b, step, rows, 0.0) + b
            if step * 2 < SEQ:
                a = a * delayed(a, step, rows, 1.0)
            step *= 2
        states[:, cols] = b.astype(BF16)
        return carry

    lax.fori_loop(0, 4, tile, 0)

    def column(n, carry):
        cols = pl.ds(pl.multiple_of(n * 512, 512), 512)
        part = jnp.dot(states[:, :256], out_own[:, cols], preferred_element_type=F32)
        part = part + jnp.dot(states[:, 256:], out_par[:, cols], preferred_element_type=F32)
        out[:, cols] = part.astype(BF16)
        return carry

    lax.fori_loop(0, 4, column, 0)


def nt_dot(a, b):
    return lax.dot_general(a, b, (((1,), (1,)), ((), ())), preferred_element_type=F32)


def tick_body(taps, out):
    out[...] = taps[...]


def up_body(x, gate, val, taps, out, buf):
    rows = lax.broadcasted_iota(jnp.int32, (SEQ, BLK), 0)
    last = 2 * HID // BLK - 1

    def product(t):
        cols = pl.ds(pl.multiple_of(t * BLK, BLK), BLK)
        return nt_dot(x[...], jnp.concatenate([gate[cols], val[cols]], axis=0))

    def finish(t, both):
        cols = pl.ds(pl.multiple_of(t * BLK, BLK), BLK)
        both = both.astype(BF16).astype(F32)
        g, v = both[:, :BLK], both[:, BLK:]
        conv = g * taps[2:3, cols]
        for k in range(2):
            conv = conv + delayed(g, 2 - k, rows, 0.0) * taps[k : k + 1, cols]
        out[:, cols] = (conv * sigmoid(conv) * v).astype(BF16)

    buf[0] = product(0)

    def tile(i, carry):
        t = 2 * i
        one = product(t + 1)
        finish(t, buf[0])
        two = product(t + 2)
        finish(t + 1, one)
        buf[0] = two
        return carry

    lax.fori_loop(0, last // 2, tile, 0)
    finish(last, buf[0])


def down_body(h, down, out):
    def tile(n, carry):
        cols = pl.ds(pl.multiple_of(n * 512, 512), 512)
        out[:, cols] = jnp.dot(h[...], down[:, cols], preferred_element_type=F32).astype(BF16)
        return carry

    lax.fori_loop(0, 4, tile, 0)


def sums_sent(part, ahead):
    return fetch(part, "y", (-ahead) % 4)


def placed(shape, blocks):
    out = jnp.zeros(shape, BF16)
    for piece, r, c in blocks:
        out = lax.dynamic_update_slice(out, piece, (r, c))
    return out


def layer(
    resid,
    mix_gain,
    in_weight,
    conv_taps,
    recur_gate_w,
    input_gate_w,
    decay_rate,
    out_weight,
    mlp_gain,
    up_gate_w,
    up_val_w,
    ffn_taps,
    down_weight,
):
    z, x = lax.axis_index("z"), lax.axis_index("x")
    steps = jnp.arange(16, dtype=jnp.int32)
    order = ((steps // 4 + z) % 4) * 4 + (steps % 4 + x) % 4

    half = sds((256 + HID + HID // 2, BLK))
    resid_rel, normed, gain2, a, b = call(
        first_body,
        [sds((SEQ, D)), sds((SEQ, D)), sds((1, D), F32), half, half],
        order,
        resid,
        mix_gain.reshape(1, D),
        mlp_gain.reshape(1, D),
        in_weight,
        out_weight,
        up_gate_w.T,
        up_val_w.T,
        down_weight,
        scalars=1,
        where=ANY,
        scratch=[
            pltpu.VMEM((SEQ, D), BF16),
            pltpu.VMEM((1, D), F32),
            pltpu.VMEM((1, D), F32),
            pltpu.SemaphoreType.DMA((11,)),
        ],
    )
    rows1 = fetch_all(normed, "y")

    a = fetch_all(a, "x")
    b = fetch_all(b, "z")
    pa = fetch_all(jnp.stack([v[:256] for v in a]), "z")
    pb = fetch_all(jnp.stack([v[:256] for v in b]), "x")
    ua = jnp.concatenate([v[256:] for v in a], axis=1)
    ub = jnp.stack([v[256:] for v in b])
    ua = fetch_all(ua, "z")
    ub = fetch_all(ub, "x")
    near = [(i, j, (4 * i + j) * BLK) for i in range(4) for j in range(4)]
    in_own = placed(
        (D, 256),
        [(pa[i][j, :BLK], at, 0) for i, j, at in near]
        + [(pb[j][i, :BLK], at, BLK) for i, j, at in near],
    )
    out_own = placed(
        (256, D),
        [(pa[i][j, BLK:], 0, at) for i, j, at in near]
        + [(pb[j][i, BLK:], BLK, at) for i, j, at in near],
    )
    in_par, out_par = partner(in_own), partner(out_own)

    (rgw, igw, small, rate, ftaps_own), _ = lax.optimization_barrier(
        ((recur_gate_w, input_gate_w, conv_taps, decay_rate[None], ffn_taps), a[1])
    )
    gates = jnp.stack(
        [
            jnp.concatenate([rgw, partner(rgw)], axis=0),
            jnp.concatenate([igw, partner(igw)], axis=0),
        ]
    ).reshape(2, 4, 2, 64, 64)
    zero = jnp.zeros_like(gates[:, :, 0])
    gates = jnp.concatenate(
        [
            jnp.concatenate([gates[:, :, 0], zero], axis=3),
            jnp.concatenate([zero, gates[:, :, 1]], axis=3),
        ],
        axis=2,
    )
    gates = jnp.concatenate([gates[0], gates[1]], axis=2)
    taps = jnp.concatenate([small, partner(small)], axis=1)
    rate = jnp.concatenate([rate, partner(rate)], axis=1)
    ftaps_par = partner(ftaps_own)
    ftaps = jnp.concatenate([ftaps_own, ftaps_par], axis=1)

    ua_par = [partner(v) for v in ua]
    ub_par = [partner(v) for v in ub]
    gate, val, down = [], [], []
    for c, (wa, wb) in enumerate(((ua, ub), (ua_par, ub_par))):
        top = c * HID
        for k in (0, 1, 3, 2):
            gate.append((wa[k][:HID], top, k * 512))
            down.append((wa[k][HID:], top, k * 512))
            for i in range(4):
                at = (4 * i + k) * BLK
                val.append((wb[k][i, :HID], top, at))
                down.append((wb[k][i, HID:], top + HID // 2, at))
    gate = placed((2 * HID, D), gate)
    val = placed((2 * HID, D), val)
    down = placed((2 * HID, D), down)

    parts = [None] * 4
    for j in (1, 3, 2, 0):
        part = call(
            mix_body,
            sds((SEQ, D)),
            rows1[j],
            in_own,
            in_par,
            taps,
            gates,
            rate,
            out_own,
            out_par,
            flops=2 * SEQ * D * 512 * 2,
            scratch=[pltpu.VMEM((SEQ, 512), BF16)] * 2,
        )
        parts[j] = sums_sent(part, j) if j else part
    middle, normed_two = call(
        second_norm_body, [sds((SEQ, D)), sds((SEQ, D))], resid_rel, *parts, gain2
    )
    rows2 = fetch_all(normed_two, "y")
    ftaps = call(tick_body, sds((3, 2 * HID), F32), ftaps)
    for j in (0, 1, 3, 2):
        hidden = call(
            up_body,
            sds((SEQ, 2 * HID)),
            rows2[j],
            gate,
            val,
            ftaps,
            flops=2 * SEQ * D * 1408 * 2,
            scratch=[pltpu.VMEM((1, SEQ, 256), F32)],
        )
        part = call(down_body, sds((SEQ, D)), hidden, down, flops=2 * SEQ * D * 1408)
        parts[j] = sums_sent(part, j) if j else part
    return call(last_sum_body, sds((SEQ, D)), order, middle, *parts, scalars=1)


def solution(mesh):
    split = Mesh(mesh.devices.reshape(4, 4, 4, 2), FS_TP)
    return jax.shard_map(
        layer,
        mesh=split,
        in_specs=(
            P(FS_TP, None),
            P(),
            P(FS, TP),
            P(None, TP),
            P(TP, None, None),
            P(TP, None, None),
            P(TP),
            P(TP, FS),
            P(),
            P(FS, TP),
            P(FS, TP),
            P(None, TP),
            P(TP, FS),
        ),
        out_specs=P(FS_TP, None),
        check_vma=False,
    )
```

```python
import jax
import jax.numpy as jnp
from jax import lax
from jax.experimental import pallas as pl
from jax.experimental.pallas import tpu as pltpu
from jax.sharding import Mesh
from jax.sharding import PartitionSpec as P


SEQ = 128
D = 2048
BLK = 128
HID = 704
F32 = jnp.float32
BF16 = jnp.bfloat16
MIB = 1024 * 1024
FS = ("z", "x")
TP = ("y", "c")
FS_TP = ("z", "x", "y", "c")


def fetch(a, axis, ahead):
    size = lax.axis_size(axis)
    return lax.ppermute(a, axis, [(i, (i - ahead) % size) for i in range(size)])


def fetch_all(a, axis):
    return [a] + [fetch(a, axis, k) for k in (1, 2, 3)]


def partner(a):
    return fetch(a, "c", 1)


VM = pl.BlockSpec(memory_space=pltpu.VMEM)
SM = pl.BlockSpec(memory_space=pltpu.SMEM)
HBM = pl.BlockSpec(memory_space=pltpu.HBM)


def call(body, out, *args, vmem=4, scalars=0, flops=0, scratch=(), where=VM, alias=None):
    return pl.pallas_call(
        body,
        in_specs=[SM] * scalars + [where] * (len(args) - scalars),
        out_specs=jax.tree.map(lambda _: VM, out),
        out_shape=out,
        scratch_shapes=scratch,
        input_output_aliases=alias or {},
        compiler_params=pltpu.CompilerParams(vmem_limit_bytes=vmem * MIB),
        cost_estimate=pl.CostEstimate(flops=flops, transcendentals=0, bytes_accessed=0),
    )(*args)


def sds(shape, dtype=BF16):
    return jax.ShapeDtypeStruct(shape, dtype)


def first_body(
    order, resid_h, gain_h, gain2_h, in_h, out_h, gate_h, val_h, down_h,
    resid_rel, normed_rel, gain2_rel, a, b, resid, gain, gain2, sems,
):
    copies = [
        pltpu.make_async_copy(src, dst, sems.at[i])
        for i, (src, dst) in enumerate(
            [
                (resid_h, resid),
                (gain_h, gain),
                (gain2_h, gain2),
                (in_h.at[:, :BLK], a.at[:BLK]),
                (in_h.at[:, BLK:], b.at[:BLK]),
                (out_h.at[:BLK], a.at[BLK : 2 * BLK]),
                (out_h.at[BLK:], b.at[BLK : 2 * BLK]),
                (gate_h, a.at[256 : 256 + HID]),
                (val_h, b.at[256 : 256 + HID]),
                (down_h.at[: HID // 2], a.at[256 + HID :]),
                (down_h.at[HID // 2 :], b.at[256 + HID :]),
            ]
        )
    ]
    for c in copies:
        c.start()
    for c in copies[:3]:
        c.wait()
    wide = resid[...].astype(F32)
    scale = lax.rsqrt(jnp.mean(wide * wide, axis=-1, keepdims=True) + 1e-06)
    for j in range(D // BLK):
        at = pl.multiple_of(order[j] * BLK, BLK)
        block = resid[:, pl.ds(at, BLK)]
        put = slice(j * BLK, (j + 1) * BLK)
        resid_rel[:, put] = block
        normed_rel[:, put] = (block.astype(F32) * scale * gain[:, pl.ds(at, BLK)]).astype(BF16)
        gain2_rel[:, put] = gain2[:, pl.ds(at, BLK)]
    for c in copies[3:]:
        c.wait()


def second_norm_body(resid, p0, p1, p2, p3, gain, middle, normed):
    total = (p0[...].astype(F32) + p1[...].astype(F32)) + (p2[...].astype(F32) + p3[...].astype(F32))
    mid = (resid[...].astype(F32) + total).astype(BF16)
    middle[...] = mid
    wide = mid.astype(F32)
    scale = lax.rsqrt(jnp.mean(wide * wide, axis=-1, keepdims=True) + 1e-06)
    normed[...] = (wide * scale * gain[...]).astype(BF16)


def last_sum_body(order, middle, p0, p1, p2, p3, out):
    for j in range(D // BLK):
        at = pl.multiple_of(order[j] * BLK, BLK)
        put = slice(j * BLK, (j + 1) * BLK)
        total = (p0[:, put].astype(F32) + p1[:, put].astype(F32)) + (
            p2[:, put].astype(F32) + p3[:, put].astype(F32)
        )
        out[:, pl.ds(at, BLK)] = (middle[:, put].astype(F32) + total).astype(BF16)


def delayed(v, steps, rows, fill):
    return jnp.where(rows >= steps, pltpu.roll(v, steps, 0), fill)


def sigmoid(v):
    return 1.0 / (1.0 + jnp.exp(-v))


def minus_expm1(v, exp_v):
    series = jnp.full_like(v, 1.0 / 9.0)
    series = 1.0 + v * series
    for k in (8.0, 7.0, 6.0, 5.0, 4.0, 3.0, 2.0):
        series = 1.0 + v * series * (1.0 / k)
    return jnp.where(v > -0.5, -v * series, 1.0 - exp_v)


def mix_body(
    x0, x1, in_own, in_par, taps, gates, rate, out_own, out_par, out0, out1, proj, states
):
    rows = lax.broadcasted_iota(jnp.int32, (2 * SEQ, BLK), 0) % SEQ
    x = jnp.concatenate([x0[...], x1[...]], axis=0)
    for half, w in enumerate((in_own, in_par)):
        proj[:, half * 256 : (half + 1) * 256] = jnp.dot(
            x, w[...], preferred_element_type=F32
        ).astype(BF16)

    def tile(t, carry):
        cols = pl.ds(pl.multiple_of(t * BLK, BLK), BLK)
        p = proj[:, cols].astype(F32)
        conv = p * taps[3:4, cols]
        for k in range(3):
            conv = conv + delayed(p, 3 - k, rows, 0.0) * taps[k : k + 1, cols]
        g = jnp.dot(conv.astype(BF16), gates[t], preferred_element_type=F32)
        rgate = sigmoid(g[:, :BLK])
        igate = sigmoid(g[:, BLK:])
        logdecay = -8.0 * rgate * rate[:, cols]
        a = jnp.exp(logdecay)
        b = jnp.sqrt(minus_expm1(2.0 * logdecay, a * a)) * (igate * conv)
        step = 1
        while step < SEQ:
            b = a * delayed(b, step, rows, 0.0) + b
            if step * 2 < SEQ:
                a = a * delayed(a, step, rows, 1.0)
            step *= 2
        states[:, cols] = b.astype(BF16)
        return carry

    lax.fori_loop(0, 4, tile, 0)

    def column(n, carry):
        cols = pl.ds(pl.multiple_of(n * 512, 512), 512)
        part = jnp.dot(states[:, :256], out_own[:, cols], preferred_element_type=F32)
        part = part + jnp.dot(states[:, 256:], out_par[:, cols], preferred_element_type=F32)
        part = part.astype(BF16)
        out0[:, cols] = part[:SEQ]
        out1[:, cols] = part[SEQ:]
        return carry

    lax.fori_loop(0, 4, column, 0)


def nt_dot(a, b):
    return lax.dot_general(a, b, (((1,), (1,)), ((), ())), preferred_element_type=F32)


ROWS = 32


def put_pieces(ks, pieces, gate, val, down):
    for n, k in enumerate(ks):
        for c in range(2):
            a, b = pieces[4 * n + 2 * c], pieces[4 * n + 2 * c + 1]
            top = c * HID
            lanes = slice(k * 512, (k + 1) * 512)

            def up_rows(r, carry):
                src = pl.ds(pl.multiple_of(r * ROWS, ROWS), ROWS)
                dst = pl.ds(pl.multiple_of(top + r * ROWS, ROWS), ROWS)
                gate[dst, lanes] = a[src]
                for i in range(4):
                    at = (4 * i + k) * BLK
                    val[dst, at : at + BLK] = b[i, src]
                return carry

            def down_rows(r, carry):
                src = pl.ds(pl.multiple_of(HID + r * ROWS, ROWS), ROWS)
                dst = pl.ds(pl.multiple_of(top + r * ROWS, ROWS), ROWS)
                low = pl.ds(pl.multiple_of(top + HID // 2 + r * ROWS, ROWS), ROWS)
                down[dst, lanes] = a[src]
                for i in range(4):
                    at = (4 * i + k) * BLK
                    down[low, at : at + BLK] = b[i, src]
                return carry

            lax.fori_loop(0, HID // ROWS, up_rows, 0)
            lax.fori_loop(0, HID // 2 // ROWS, down_rows, 0)


def early_body(*refs):
    put_pieces((0, 1, 3), refs[:12], *refs[12:])


def late_body(*refs):
    put_pieces((2,), refs[:4], *refs[7:])


def up_body(x0, x1, gate, val, taps, out, buf):
    rows = lax.broadcasted_iota(jnp.int32, (2 * SEQ, BLK), 0) % SEQ
    last = 2 * HID // BLK - 1

    def product(t):
        cols = pl.ds(pl.multiple_of(t * BLK, BLK), BLK)
        x = jnp.concatenate([x0[...], x1[...]], axis=0)
        return nt_dot(x, jnp.concatenate([gate[cols], val[cols]], axis=0))

    def finish(t, both):
        cols = pl.ds(pl.multiple_of(t * BLK, BLK), BLK)
        both = both.astype(BF16).astype(F32)
        g, v = both[:, :BLK], both[:, BLK:]
        conv = g * taps[2:3, cols]
        for k in range(2):
            conv = conv + delayed(g, 2 - k, rows, 0.0) * taps[k : k + 1, cols]
        out[:, cols] = (conv * sigmoid(conv) * v).astype(BF16)

    buf[...] = product(0)

    def tile(i, carry):
        t = 2 * i
        one = product(t + 1)
        finish(t, buf[...])
        two = product(t + 2)
        finish(t + 1, one)
        buf[...] = two
        return carry

    lax.fori_loop(0, last // 2, tile, 0)
    finish(last, buf[...])


def down_body(h, down, out0, out1):
    def tile(n, carry):
        cols = pl.ds(pl.multiple_of(n * 512, 512), 512)
        part = jnp.dot(h[...], down[:, cols], preferred_element_type=F32).astype(BF16)
        out0[:, cols] = part[:SEQ]
        out1[:, cols] = part[SEQ:]
        return carry

    lax.fori_loop(0, 4, tile, 0)


def sums_sent(part, ahead):
    return fetch(part, "y", (-ahead) % 4)


def placed(shape, blocks):
    out = jnp.zeros(shape, BF16)
    for piece, r, c in blocks:
        out = lax.dynamic_update_slice(out, piece, (r, c))
    return out


def layer(
    resid,
    mix_gain,
    in_weight,
    conv_taps,
    recur_gate_w,
    input_gate_w,
    decay_rate,
    out_weight,
    mlp_gain,
    up_gate_w,
    up_val_w,
    ffn_taps,
    down_weight,
):
    z, x = lax.axis_index("z"), lax.axis_index("x")
    steps = jnp.arange(16, dtype=jnp.int32)
    order = ((steps // 4 + z) % 4) * 4 + (steps % 4 + x) % 4

    half = sds((256 + HID + HID // 2, BLK))
    resid_rel, normed, gain2, a, b = call(
        first_body,
        [sds((SEQ, D)), sds((SEQ, D)), sds((1, D), F32), half, half],
        order,
        resid,
        mix_gain.reshape(1, D),
        mlp_gain.reshape(1, D),
        in_weight,
        out_weight,
        up_gate_w.T,
        up_val_w.T,
        down_weight,
        scalars=1,
        where=HBM,
        scratch=[
            pltpu.VMEM((SEQ, D), BF16),
            pltpu.VMEM((1, D), F32),
            pltpu.VMEM((1, D), F32),
            pltpu.SemaphoreType.DMA((11,)),
        ],
    )
    rows1 = fetch_all(normed, "y")

    a = fetch_all(a, "x")
    b = fetch_all(b, "z")
    pa = fetch_all(jnp.stack([v[:256] for v in a]), "z")
    pb = fetch_all(jnp.stack([v[:256] for v in b]), "x")
    ua = jnp.concatenate([v[256:] for v in a], axis=1)
    ub = jnp.stack([v[256:] for v in b])
    ua = fetch_all(ua, "z")
    ub = fetch_all(ub, "x")
    near = [(i, j, (4 * i + j) * BLK) for i in range(4) for j in range(4)]
    in_own = placed(
        (D, 256),
        [(pa[i][j, :BLK], at, 0) for i, j, at in near]
        + [(pb[j][i, :BLK], at, BLK) for i, j, at in near],
    )
    out_own = placed(
        (256, D),
        [(pa[i][j, BLK:], 0, at) for i, j, at in near]
        + [(pb[j][i, BLK:], BLK, at) for i, j, at in near],
    )
    in_par, out_par = partner(in_own), partner(out_own)

    (rgw, igw, small, rate, ftaps_own), _ = lax.optimization_barrier(
        ((recur_gate_w, input_gate_w, conv_taps, decay_rate[None], ffn_taps), a[1])
    )
    gates = jnp.stack(
        [
            jnp.concatenate([rgw, partner(rgw)], axis=0),
            jnp.concatenate([igw, partner(igw)], axis=0),
        ]
    ).reshape(2, 4, 2, 64, 64)
    zero = jnp.zeros_like(gates[:, :, 0])
    gates = jnp.concatenate(
        [
            jnp.concatenate([gates[:, :, 0], zero], axis=3),
            jnp.concatenate([zero, gates[:, :, 1]], axis=3),
        ],
        axis=2,
    )
    gates = jnp.concatenate([gates[0], gates[1]], axis=2)
    taps = jnp.concatenate([small, partner(small)], axis=1)
    rate = jnp.concatenate([rate, partner(rate)], axis=1)
    ftaps_par = partner(ftaps_own)
    ftaps = jnp.concatenate([ftaps_own, ftaps_par], axis=1)

    ua_par = [partner(v) for v in ua]
    ub_par = [partner(v) for v in ub]

    parts = [None] * 4
    for i, j in ((1, 3), (2, 0)):
        pair = call(
            mix_body,
            [sds((SEQ, D))] * 2,
            rows1[i],
            rows1[j],
            in_own,
            in_par,
            taps,
            gates,
            rate,
            out_own,
            out_par,
            flops=2 * 2 * SEQ * D * 512 * 2,
            scratch=[pltpu.VMEM((2 * SEQ, 512), BF16)] * 2,
        )
        for k, part in zip((i, j), pair):
            parts[k] = sums_sent(part, k) if k else part
    middle, normed_two = call(
        second_norm_body, [sds((SEQ, D)), sds((SEQ, D))], resid_rel, *parts, gain2
    )
    rows2 = fetch_all(normed_two, "y")

    whole = [sds((2 * HID, D))] * 3

    def pieces(*ks):
        return [v[k] for k in ks for v in (ua, ub, ua_par, ub_par)]

    weights = call(early_body, whole, *pieces(0, 1, 3))
    weights = call(late_body, whole, *pieces(2), *weights, alias={4: 0, 5: 1, 6: 2})
    gate, val, down = weights

    for i, j in ((1, 3), (2, 0)):
        hidden = call(
            up_body,
            sds((2 * SEQ, 2 * HID)),
            rows2[i],
            rows2[j],
            gate,
            val,
            ftaps,
            flops=2 * 2 * SEQ * D * 1408 * 2,
            scratch=[pltpu.VMEM((2 * SEQ, 256), F32)],
        )
        pair = call(
            down_body, [sds((SEQ, D))] * 2, hidden, down, flops=2 * 2 * SEQ * D * 1408
        )
        for k, part in zip((i, j), pair):
            parts[k] = sums_sent(part, k) if k else part
    return call(last_sum_body, sds((SEQ, D)), order, middle, *parts, scalars=1)


def solution(mesh):
    split = Mesh(mesh.devices.reshape(4, 4, 4, 2), FS_TP)
    return jax.shard_map(
        layer,
        mesh=split,
        in_specs=(
            P(FS_TP, None),
            P(),
            P(FS, TP),
            P(None, TP),
            P(TP, None, None),
            P(TP, None, None),
            P(TP),
            P(TP, FS),
            P(),
            P(FS, TP),
            P(FS, TP),
            P(None, TP),
            P(TP, FS),
        ),
        out_specs=P(FS_TP, None),
        check_vma=False,
    )
```
